32 devices in a mesh: ep: 32 (over z, y, x, core).
Axes of the slice: x: 2, y: 2, z: 4, core: 2. Of those that a mesh axis runs over, the one named last changes fastest.
Arguments:
- tokens: bfloat16 [768, 2048], P('ep'), may hold values from -6 to 6
- lengths: int32 [768], P('ep'), may hold values from 2 to 1024
- latent_cache: bfloat16 [768, 1024, 256], P('ep'), may hold values from -500 to 500
- rotary_cache: bfloat16 [768, 1024, 32], P('ep'), may hold values from -6 to 6
- route_ids: int32 [768, 6], P('ep'), may hold values from 0 to 31, all different within a row; in each aligned block of 24 rows (0 to 23, 24 to 47, ...) at most 12 rows name the same one
- route_scores: float32 [768, 6], P('ep'), may hold values from 0.05 to 1
- attn_gain: bfloat16 [2048], replicated, may hold values from 0.099609375 to 1.8984375
- w_query_down: bfloat16 [2048, 256], replicated, may hold values from -0.125 to 0.125
- query_gain: bfloat16 [256], replicated, may hold values from 0.099609375 to 1.8984375
- w_query_nope: bfloat16 [256, 2048], replicated, may hold values from -0.375 to 0.375
- w_query_rope: bfloat16 [256, 1024], replicated, may hold values from -0.375 to 0.375
- w_key_absorb: bfloat16 [32, 64, 256], replicated, may hold values from -0.75 to 0.75
- latent_gain: bfloat16 [256], replicated, may hold values from 0.099609375 to 1.8984375
- w_latent_down: bfloat16 [2048, 256], replicated, may hold values from -0.125 to 0.125
- w_rotary_key: bfloat16 [2048, 32], replicated, may hold values from -0.125 to 0.125
- w_value_up: bfloat16 [32, 256, 64], replicated, may hold values from -0.375 to 0.375
- w_output: bfloat16 [2048, 2048], P(None, 'ep'), may hold values from -0.125 to 0.125
- ffn_gain: bfloat16 [2048], replicated, may hold values from 0.099609375 to 1.8984375
- expert_gate: bfloat16 [32, 2048, 512], P('ep'), may hold values from -0.125 to 0.125
- expert_up: bfloat16 [32, 2048, 512], P('ep'), may hold values from -0.125 to 0.125
- expert_down: bfloat16 [32, 512, 2048], P('ep'), may hold values from -0.25 to 0.25
- shared_gate: bfloat16 [2048, 256], replicated, may hold values from -0.125 to 0.125
- shared_up: bfloat16 [2048, 256], replicated, may hold values from -0.125 to 0.125
- shared_down: bfloat16 [256, 2048], replicated, may hold values from -0.375 to 0.375
Outputs:
- mixed: bfloat16 [768, 2048], P('ep')
- latent_new: bfloat16 [768, 256], P('ep')
- rotary_new: bfloat16 [768, 32], P('ep')
The draws below stay inside these ranges and needn't reach their ends.
Inputs may be any that keep to these rules, and one draw needn't show every extreme that they name: `route_ids`: within the rows of one device no expert is named by more than 12 rows, a bound that some block reaches; each row names 6 different experts. `lengths`: cache positions at or past a sequence's length are not read.
All inputs are finite; a program needn't handle non-finite values.
Results may differ from the reference program's by a relative error of at most 0.025.
Values may be sent and summed in bfloat16 or wider, within the bound.
A program may use at most 128 MiB of HBM per device.

```python
import math
import jax
import jax.numpy as jnp
import numpy as np
from jax import lax

D = 2048
HEADS = 32
NOPE = 64
ROPE = 32
VDIM = 64
QRANK = 256
LAT = 256
EH = 512
SH = 256
TOP = 6
B_DEV = 24
CACHE = 1024
SEQS = 768
EXPERTS = 32
CAP = 12
N_EP = 32


def draw_latent_cache(key, part):
    base = jnp.clip(jax.random.normal(jax.random.fold_in(key, 11), (SEQS, CACHE, LAT), jnp.float32), -6.0, 6.0)
    return base.astype(jnp.bfloat16)


def place_ends(drawn, rng, least, top_value):
    longest = drawn.shape.index(max(drawn.shape))
    spots = []
    for shift in (0, 1):
        where = [jax.random.randint(jax.random.fold_in(rng, axis), (), 0, length) for axis, length in enumerate(drawn.shape)]
        where[longest] = (where[longest] + shift) % drawn.shape[longest]
        spots.append(tuple(where))
    return drawn.at[spots[0]].set(least).at[spots[1]].set(top_value)


def shard_levels(own_key, shape, split, low, top_value):
    loudness = 1.0
    for dim, shards_of in split:
        heights = jax.random.uniform(jax.random.fold_in(jax.random.fold_in(own_key, 6), dim), (shards_of,), jnp.float32, low / len(split), top_value / len(split))
        loudness = loudness * jnp.repeat(jnp.exp(heights), shape[dim] // shards_of).reshape((-1,) + (1,) * (len(shape) - 1 - dim))
    return loudness


def routed_block(rng, own, number, rows, amount, top, most, lean):
    ranking = jax.random.permutation(rng, amount)
    crowded, ordinary = load_shares(amount, rows * top, most, lean, True), load_shares(amount, rows * top, most, lean, False)
    places = jnp.arange(amount)

    def named(tallies, turn):
        used = int((tallies > 0).sum())
        fixed = max(1, used // 4)
        passed = fixed + (places - fixed + turn * (used - fixed)) % max(1, amount - fixed)
        return jnp.zeros((amount,), jnp.int32).at[ranking[jnp.where(places < fixed, places, passed)]].set(jnp.asarray(tallies, jnp.int32))

    tallies = jnp.where(number % 4 == 0, named(crowded, number // 4), named(ordinary, number - number // 4 - 1))
    mixed = jax.random.permutation(jax.random.fold_in(own, 3), amount)
    donor, sink = mixed[0:amount // 2 * 2:2], mixed[1:amount // 2 * 2:2]
    margin = jnp.minimum(tallies[donor] - 1, most - tallies[sink]) // 2
    margin = jnp.where((donor == ranking[0]) | (sink == ranking[0]) | (tallies[sink] == 0), 0, jnp.maximum(margin, 0))
    passed = jax.random.randint(jax.random.fold_in(own, 4), (amount // 2,), 0, 1 << 20) % (margin + 1)
    tallies = tallies.at[donor].add(-passed).at[sink].add(passed)
    items = jnp.searchsorted(jnp.cumsum(tallies), jnp.arange(rows * top), side="right").astype(jnp.int32)
    grid = items.reshape(top, rows).T
    grid = grid[jax.random.permutation(jax.random.fold_in(own, 1), rows)]
    turn = jax.random.randint(jax.random.fold_in(own, 2), (rows, 1), 0, top)
    return jnp.take_along_axis(grid, (jnp.arange(top)[None, :] + turn) % top, axis=1)


def load_shares(count, total, most, skew, full):
    loads = [(1 << 20) // math.isqrt(rank ** skew) + 1 for rank in range(1, count + 1)]
    largest = most if full else min(most, max(-(-total // count), total * loads[0] // sum(loads)))
    least = 1 if total - largest >= count - 1 else 0
    given, spare = [largest] + [least] * (count - 1), total - largest - least * (count - 1)
    while spare > 0:
        movable = [i for i in range(1, count) if given[i] < largest] or [i for i in range(1, count) if given[i] < most]
        mass, budget = sum([loads[i] for i in movable]), spare
        for i in movable:
            more = min(most - given[i], max(1, budget * loads[i] // mass), spare)
            given[i] = given[i] + more
            spare = spare - more
    return np.array(given)


def noise(own_key, extent, spread, limit, split=(), held_as=jnp.bfloat16):
    drawn = spread * jax.random.normal(own_key, extent, jnp.float32)
    if split:
        drawn = drawn * shard_levels(own_key, extent, split, -0.22, 0.18)
    return jnp.clip(drawn, -limit, limit).astype(held_as)


def setup_inputs(seed: int = 0) -> dict:
    keys = jax.random.split(jax.random.key(seed), 25)
    tokens = noise(keys[0], (SEQS, D), 1.0, 6.0, ((0, 32),))
    lengths = place_ends(jax.random.randint(keys[1], (SEQS,), 2, CACHE + 1), jax.random.fold_in(keys[1], 1), 2, CACHE).astype(jnp.int32)
    latent_cache = draw_latent_cache(jax.random.fold_in(keys[24], 71), 0)
    rotary_cache = noise(keys[3], (SEQS, CACHE, ROPE), 1.0, 6.0, ((0, 32),))
    route_ids_keys = jax.random.split(jax.random.fold_in(keys[4], 1), SEQS // B_DEV)
    route_ids_turns = jax.random.permutation(jax.random.fold_in(keys[4], 3), SEQS // B_DEV)
    route_ids = jax.vmap(lambda own, number: routed_block(jax.random.fold_in(keys[4], 2), own, number, B_DEV, EXPERTS, TOP, CAP, 2))(route_ids_keys, route_ids_turns).reshape((SEQS, TOP))
    route_scores = jnp.clip(0.05 + 0.95 * jax.random.uniform(keys[5], (SEQS, TOP), jnp.float32) ** shard_levels(keys[5], (SEQS, TOP), ((0, 32),), -0.2, 0.2), 0.05, 1.0)
    attn_gain = jnp.clip(1.0 + 0.18 * jax.random.normal(keys[6], (D,), jnp.float32), 0.099609375, 1.8984375).astype(jnp.bfloat16)
    w_query_down = noise(keys[7], (D, QRANK), D ** -0.5, 0.125)
    query_gain = jnp.clip(1.0 + 0.18 * jax.random.normal(keys[8], (QRANK,), jnp.float32), 0.099609375, 1.8984375).astype(jnp.bfloat16)
    w_query_nope = noise(keys[9], (QRANK, HEADS * NOPE), QRANK ** -0.5, 0.375)
    w_query_rope = noise(keys[10], (QRANK, HEADS * ROPE), QRANK ** -0.5, 0.375)
    w_key_absorb = noise(keys[11], (HEADS, NOPE, LAT), NOPE ** -0.5, 0.75)
    latent_gain = jnp.clip(1.0 + 0.18 * jax.random.normal(keys[12], (LAT,), jnp.float32), 0.099609375, 1.8984375).astype(jnp.bfloat16)
    w_latent_down = noise(keys[13], (D, LAT), D ** -0.5, 0.125)
    w_rotary_key = noise(keys[14], (D, ROPE), D ** -0.5, 0.125)
    w_value_up = noise(keys[15], (HEADS, LAT, VDIM), LAT ** -0.5, 0.375)
    w_output = noise(keys[16], (D, D), D ** -0.5, 0.125, ((1, 32),))
    ffn_gain = jnp.clip(1.0 + 0.18 * jax.random.normal(keys[17], (D,), jnp.float32), 0.099609375, 1.8984375).astype(jnp.bfloat16)
    expert_gate = noise(keys[18], (EXPERTS, D, EH), D ** -0.5, 0.125, ((0, 32),))
    expert_up = noise(keys[19], (EXPERTS, D, EH), D ** -0.5, 0.125, ((0, 32),))
    expert_down = noise(keys[20], (EXPERTS, EH, D), EH ** -0.5, 0.25, ((0, 32),))
    shared_gate = noise(keys[21], (D, SH), D ** -0.5, 0.125)
    shared_up = noise(keys[22], (D, SH), D ** -0.5, 0.125)
    shared_down = noise(keys[23], (SH, D), SH ** -0.5, 0.375)
    return dict(tokens=tokens, lengths=lengths, latent_cache=latent_cache, rotary_cache=rotary_cache, route_ids=route_ids, route_scores=route_scores, attn_gain=attn_gain, w_query_down=w_query_down, query_gain=query_gain, w_query_nope=w_query_nope, w_query_rope=w_query_rope, w_key_absorb=w_key_absorb, latent_gain=latent_gain, w_latent_down=w_latent_down, w_rotary_key=w_rotary_key, w_value_up=w_value_up, w_output=w_output, ffn_gain=ffn_gain, expert_gate=expert_gate, expert_up=expert_up, expert_down=expert_down, shared_gate=shared_gate, shared_up=shared_up, shared_down=shared_down)


EPSILON = 1e-06
THETA = 10000.0
ROUTED_SCALE = 2.5

def rms_scale(values, gain):
    squares = lax.optimization_barrier(jnp.mean(values * values, axis=-1, keepdims=True))
    return values * lax.rsqrt(squares + EPSILON) * gain.astype(jnp.float32)

def rotate(values, positions):
    half = values.shape[-1] // 2
    freqs = 1.0 / THETA ** (jnp.arange(half, dtype=jnp.float32) * 2.0 / values.shape[-1])
    angles = positions.astype(jnp.float32)[:, None] * freqs[None, :]
    if values.ndim == 3:
        angles = angles[:, None, :]
    cosine, sine = (jnp.cos(angles), jnp.sin(angles))
    first, second = (values[..., :half], values[..., half:])
    return jnp.concatenate([first * cosine - second * sine, second * cosine + first * sine], axis=-1)

def attend_block(tokens, lengths, latent_cache, rotary_cache, attn_gain, w_query_down, query_gain, w_query_nope, w_query_rope, w_key_absorb, latent_gain, w_latent_down, w_rotary_key, w_value_up):
    f32 = jnp.float32
    rows = tokens.shape[0]
    heads, nope, latent = w_key_absorb.shape
    rotary = w_rotary_key.shape[1]
    normed = rms_scale(tokens.astype(f32), attn_gain).astype(jnp.bfloat16)
    query_low = rms_scale(jnp.dot(normed, w_query_down, preferred_element_type=f32), query_gain).astype(jnp.bfloat16)
    query_nope = jnp.dot(query_low, w_query_nope, preferred_element_type=f32).astype(jnp.bfloat16).reshape(rows, heads, nope)
    query_rot = jnp.dot(query_low, w_query_rope, preferred_element_type=f32).reshape(rows, heads, rotary)
    query_rot = rotate(query_rot, lengths).astype(jnp.bfloat16)
    query_lat = jnp.einsum('thn,hnl->thl', query_nope.astype(f32), w_key_absorb.astype(f32)).astype(jnp.bfloat16)
    latent_new = rms_scale(jnp.dot(normed, w_latent_down, preferred_element_type=f32), latent_gain).astype(jnp.bfloat16)
    rotary_new = rotate(jnp.dot(normed, w_rotary_key, preferred_element_type=f32), lengths).astype(jnp.bfloat16)
    scale = (nope + rotary) ** (-0.5)
    scores = (jnp.einsum('thl,tkl->thk', query_lat.astype(f32), latent_cache.astype(f32)) + jnp.einsum('thr,tkr->thk', query_rot.astype(f32), rotary_cache.astype(f32))) * scale
    live = jnp.arange(latent_cache.shape[1], dtype=jnp.int32)[None, :] < lengths[:, None]
    scores = jnp.where(live[:, None, :], scores, -jnp.inf)
    own = (jnp.einsum('thl,tl->th', query_lat.astype(f32), latent_new.astype(f32)) + jnp.einsum('thr,tr->th', query_rot.astype(f32), rotary_new.astype(f32))) * scale
    top = jnp.maximum(lax.optimization_barrier(jnp.max(scores, axis=-1)), own)
    weights = jnp.exp(scores - top[..., None])
    own_weight = jnp.exp(own - top)
    total = lax.optimization_barrier(jnp.sum(weights, axis=-1)) + own_weight
    probs = (weights / total[..., None]).astype(jnp.bfloat16)
    own_prob = (own_weight / total).astype(jnp.bfloat16)
    out_lat = jnp.einsum('thk,tkl->thl', probs.astype(f32), latent_cache.astype(f32))
    out_lat = (out_lat + own_prob.astype(f32)[..., None] * latent_new.astype(f32)[:, None, :]).astype(jnp.bfloat16)
    values = jnp.einsum('thl,hlv->thv', out_lat.astype(f32), w_value_up.astype(f32)).astype(jnp.bfloat16)
    return (values.reshape(rows, heads * w_value_up.shape[2]), latent_new, rotary_new)

def reference(tokens, lengths, latent_cache, rotary_cache, route_ids, route_scores, attn_gain, w_query_down, query_gain, w_query_nope, w_query_rope, w_key_absorb, latent_gain, w_latent_down, w_rotary_key, w_value_up, w_output, ffn_gain, expert_gate, expert_up, expert_down, shared_gate, shared_up, shared_down):
    f32 = jnp.float32

    def one_block(pieces):
        return attend_block(pieces[0], pieces[1], pieces[2], pieces[3], attn_gain, w_query_down, query_gain, w_query_nope, w_query_rope, w_key_absorb, latent_gain, w_latent_down, w_rotary_key, w_value_up)
    values, latent_new, rotary_new = lax.map(one_block, (tokens.reshape(N_EP, B_DEV, D), lengths.reshape(N_EP, B_DEV), latent_cache.reshape(N_EP, B_DEV, CACHE, LAT), rotary_cache.reshape(N_EP, B_DEV, CACHE, ROPE)))
    values = values.reshape(SEQS, D)
    latent_new = latent_new.reshape(SEQS, LAT)
    rotary_new = rotary_new.reshape(SEQS, ROPE)
    attended = jnp.dot(values, w_output, preferred_element_type=f32).astype(jnp.bfloat16)
    residual = (tokens.astype(f32) + attended.astype(f32)).astype(jnp.bfloat16)
    ffn_in = rms_scale(residual.astype(f32), ffn_gain).astype(jnp.bfloat16)
    blocks = route_ids.reshape(N_EP, B_DEV * TOP)
    hits = (blocks[:, :, None] == jnp.arange(EXPERTS, dtype=jnp.int32)[None, None, :]).astype(jnp.int32)
    earlier = jnp.cumsum(hits, axis=1) - hits
    slot = lax.optimization_barrier(jnp.sum(earlier * hits, axis=2))
    global_slot = (jnp.arange(N_EP, dtype=jnp.int32)[:, None] * CAP + slot).reshape(-1)
    flat_ids = blocks.reshape(-1)
    pair_index = jnp.arange(SEQS * TOP, dtype=jnp.int32)
    table = jnp.full((EXPERTS, N_EP * CAP), SEQS * TOP, jnp.int32).at[flat_ids, global_slot].set(pair_index)
    padded = jnp.concatenate([jnp.repeat(ffn_in, TOP, axis=0), jnp.zeros((1, D), jnp.bfloat16)], axis=0)

    def one_expert(pieces):
        index, gate_w, up_w, down_w = pieces
        rows = padded[index]
        gate = jnp.dot(rows, gate_w, preferred_element_type=f32)
        upward = jnp.dot(rows, up_w, preferred_element_type=f32)
        hidden = (jax.nn.silu(gate) * upward).astype(jnp.bfloat16)
        return jnp.dot(hidden, down_w, preferred_element_type=f32).astype(jnp.bfloat16)
    outputs = lax.map(one_expert, (table, expert_gate, expert_up, expert_down))
    picked = outputs[flat_ids, global_slot].astype(f32).reshape(SEQS, TOP, D)
    route_weight = ROUTED_SCALE * route_scores / lax.optimization_barrier(jnp.sum(route_scores, axis=1, keepdims=True))
    routed = lax.optimization_barrier(jnp.sum(picked * route_weight[:, :, None], axis=1))
    gate_s = jnp.dot(ffn_in, shared_gate, preferred_element_type=f32)
    up_s = jnp.dot(ffn_in, shared_up, preferred_element_type=f32)
    hidden_s = (jax.nn.silu(gate_s) * up_s).astype(jnp.bfloat16)
    shared_out = jnp.dot(hidden_s, shared_down, preferred_element_type=f32)
    mixed = (residual.astype(f32) + routed + shared_out).astype(jnp.bfloat16)
    return (mixed, latent_new, rotary_new)
```

```python
import jax
import jax.numpy as jnp
from jax import lax
from jax.sharding import PartitionSpec as P

EPSILON = 1e-06
THETA = 10000.0
ROUTED_SCALE = 2.5


def rms_scale(values, gain):
    squares = jnp.mean(values * values, axis=-1, keepdims=True)
    return values * lax.rsqrt(squares + EPSILON) * gain.astype(jnp.float32)


def rotate(values, positions):
    half = values.shape[-1] // 2
    freqs = 1.0 / THETA ** (jnp.arange(half, dtype=jnp.float32) * 2.0 / values.shape[-1])
    angles = positions.astype(jnp.float32)[:, None] * freqs[None, :]
    if values.ndim == 3:
        angles = angles[:, None, :]
    cosine, sine = (jnp.cos(angles), jnp.sin(angles))
    first, second = (values[..., :half], values[..., half:])
    return jnp.concatenate(
        [first * cosine - second * sine, second * cosine + first * sine], axis=-1
    )


def shards(
    tokens,
    lengths,
    latent_cache,
    rotary_cache,
    route_ids,
    route_scores,
    attn_gain,
    w_query_down,
    query_gain,
    w_query_nope,
    w_query_rope,
    w_key_absorb,
    latent_gain,
    w_latent_down,
    w_rotary_key,
    w_value_up,
    w_output,
    ffn_gain,
    expert_gate,
    expert_up,
    expert_down,
    shared_gate,
    shared_up,
    shared_down,
):
    f32 = jnp.float32
    bf16 = jnp.bfloat16
    rows, model = tokens.shape
    heads, nope, latent = w_key_absorb.shape
    rotary = w_rotary_key.shape[1]
    normed = rms_scale(tokens.astype(f32), attn_gain).astype(bf16)
    query_low = rms_scale(
        jnp.dot(normed, w_query_down, preferred_element_type=f32), query_gain
    ).astype(bf16)
    query_nope = (
        jnp.dot(query_low, w_query_nope, preferred_element_type=f32)
        .astype(bf16)
        .reshape(rows, heads, nope)
    )
    query_rot = jnp.dot(query_low, w_query_rope, preferred_element_type=f32).reshape(
        rows, heads, rotary
    )
    query_rot = rotate(query_rot, lengths).astype(bf16)
    query_lat = jnp.einsum(
        "thn,hnl->thl", query_nope, w_key_absorb, preferred_element_type=f32
    ).astype(bf16)
    latent_new = rms_scale(
        jnp.dot(normed, w_latent_down, preferred_element_type=f32), latent_gain
    ).astype(bf16)
    rotary_new = rotate(jnp.dot(normed, w_rotary_key, preferred_element_type=f32), lengths).astype(
        bf16
    )
    scale = (nope + rotary) ** (-0.5)
    scores = (
        jnp.einsum("thl,tkl->thk", query_lat, latent_cache, preferred_element_type=f32)
        + jnp.einsum("thr,tkr->thk", query_rot, rotary_cache, preferred_element_type=f32)
    ) * scale
    live = jnp.arange(latent_cache.shape[1], dtype=jnp.int32)[None, :] < lengths[:, None]
    scores = jnp.where(live[:, None, :], scores, -jnp.inf)
    own = (
        jnp.einsum("thl,tl->th", query_lat, latent_new, preferred_element_type=f32)
        + jnp.einsum("thr,tr->th", query_rot, rotary_new, preferred_element_type=f32)
    ) * scale
    highest = jnp.maximum(jnp.max(scores, axis=-1), own)
    weights = jnp.exp(scores - highest[..., None])
    own_weight = jnp.exp(own - highest)
    total = jnp.sum(weights, axis=-1) + own_weight
    probs = (weights / total[..., None]).astype(bf16)
    own_prob = (own_weight / total).astype(bf16)
    out_lat = jnp.einsum("thk,tkl->thl", probs, latent_cache, preferred_element_type=f32)
    out_lat = (
        out_lat + own_prob.astype(f32)[..., None] * latent_new.astype(f32)[:, None, :]
    ).astype(bf16)
    values = jnp.einsum("thl,hlv->thv", out_lat, w_value_up, preferred_element_type=f32).astype(
        bf16
    )
    values = values.reshape(rows, model)
    devices = lax.axis_size("ep")
    me = lax.axis_index("ep")
    local_experts = expert_gate.shape[0]
    experts = devices * local_experts
    route_weight = ROUTED_SCALE * route_scores / jnp.sum(route_scores, axis=1, keepdims=True)
    chosen = route_ids[:, :, None] == jnp.arange(experts, dtype=jnp.int32)[None, None, :]
    share = jnp.sum(jnp.where(chosen, route_weight[:, :, None], 0.0), axis=1)
    share_high = share.astype(bf16)
    share_low = (share - share_high.astype(f32)).astype(bf16)
    packed = jnp.concatenate([values, share_high, share_low], axis=1)
    everyone = lax.all_gather(packed, "ep", axis=0, tiled=True)
    column_part = jnp.dot(everyone[:, :model], w_output, preferred_element_type=f32).astype(bf16)
    attended = lax.all_to_all(column_part, "ep", split_axis=0, concat_axis=1, tiled=True)
    residual = (tokens.astype(f32) + attended.astype(f32)).astype(bf16)
    ffn_in = rms_scale(residual.astype(f32), ffn_gain).astype(bf16)
    every_in = lax.all_gather(ffn_in, "ep", axis=0, tiled=True)
    partial = jnp.zeros((devices * rows, model), f32)
    for j in range(local_experts):
        number = me * local_experts + j
        weight = lax.dynamic_slice_in_dim(everyone, model + number, 1, 1).astype(
            f32
        ) + lax.dynamic_slice_in_dim(everyone, model + experts + number, 1, 1).astype(f32)
        gate = jnp.dot(every_in, expert_gate[j], preferred_element_type=f32)
        upward = jnp.dot(every_in, expert_up[j], preferred_element_type=f32)
        hidden = (jax.nn.silu(gate) * upward).astype(bf16)
        result = jnp.dot(hidden, expert_down[j], preferred_element_type=f32).astype(bf16)
        partial = partial + result.astype(f32) * weight
    routed = lax.psum_scatter(
        partial.astype(bf16), "ep", scatter_dimension=0, tiled=True
    ).astype(f32)
    gate_shared = jnp.dot(ffn_in, shared_gate, preferred_element_type=f32)
    up_shared = jnp.dot(ffn_in, shared_up, preferred_element_type=f32)
    hidden_shared = (jax.nn.silu(gate_shared) * up_shared).astype(bf16)
    shared_out = jnp.dot(hidden_shared, shared_down, preferred_element_type=f32)
    mixed = (residual.astype(f32) + routed + shared_out).astype(bf16)
    return (mixed, latent_new, rotary_new)


def solution(mesh):
    return jax.shard_map(
        shards,
        mesh=mesh,
        in_specs=(
            P("ep", None),
            P("ep"),
            P("ep", None, None),
            P("ep", None, None),
            P("ep", None),
            P("ep", None),
            P(),
            P(),
            P(),
            P(),
            P(),
            P(),
            P(),
            P(),
            P(),
            P(),
            P(None, "ep"),
            P(),
            P("ep", None, None),
            P("ep", None, None),
            P("ep", None, None),
            P(),
            P(),
            P(),
        ),
        out_specs=(P("ep", None), P("ep", None), P("ep", None)),
        check_vma=False,
    )
```

```python
import jax
import jax.numpy as jnp
from jax import lax
from jax.experimental import pallas as pl
from jax.experimental.pallas import tpu as pltpu
from jax.sharding import PartitionSpec as P

EPSILON = 1e-06
THETA = 10000.0
ROUTED_SCALE = 2.5


def rms_scale(values, gain):
    squares = jnp.mean(values * values, axis=-1, keepdims=True)
    return values * lax.rsqrt(squares + EPSILON) * gain.astype(jnp.float32)


def rotate(values, positions):
    half = values.shape[-1] // 2
    freqs = 1.0 / THETA ** (jnp.arange(half, dtype=jnp.float32) * 2.0 / values.shape[-1])
    angles = positions.astype(jnp.float32)[:, None] * freqs[None, :]
    if values.ndim == 3:
        angles = angles[:, None, :]
    cosine, sine = (jnp.cos(angles), jnp.sin(angles))
    first, second = (values[..., :half], values[..., half:])
    return jnp.concatenate(
        [first * cosine - second * sine, second * cosine + first * sine], axis=-1
    )


def exchange_kernel(n, src, dst, send_sem, recv_sem, local_sem):
    me = lax.axis_index("ep")
    barrier = pltpu.get_barrier_semaphore()

    def greet(i, carry):
        pl.semaphore_signal(
            barrier,
            inc=1,
            device_id=(lax.rem(me + i, n),),
            device_id_type=pl.DeviceIdType.MESH,
        )
        return carry

    lax.fori_loop(1, n, greet, 0)
    pl.semaphore_wait(barrier, n - 1)
    own = pltpu.make_async_copy(src.at[me], dst.at[me], local_sem)
    own.start()

    def send(i, carry):
        peer = lax.rem(me + i, n)
        pltpu.make_async_remote_copy(
            src_ref=src.at[peer],
            dst_ref=dst.at[me],
            send_sem=send_sem.at[i],
            recv_sem=recv_sem.at[i],
            device_id=(peer,),
            device_id_type=pl.DeviceIdType.MESH,
        ).start()
        return carry

    lax.fori_loop(1, n, send, 0)

    def finish(i, carry):
        peer = lax.rem(me + i, n)
        sender = lax.rem(me + n - i, n)
        copy = pltpu.make_async_remote_copy(
            src_ref=src.at[peer],
            dst_ref=dst.at[sender],
            send_sem=send_sem.at[i],
            recv_sem=recv_sem.at[i],
            device_id=(peer,),
            device_id_type=pl.DeviceIdType.MESH,
        )
        copy.wait_send()
        copy.wait_recv()
        return carry

    lax.fori_loop(1, n, finish, 0)
    own.wait()


def exchange(blocks, number):
    n = blocks.shape[0]
    dense = blocks.reshape(n, -1, 128)
    return pl.pallas_call(
        lambda *refs: exchange_kernel(n, *refs),
        out_shape=jax.ShapeDtypeStruct(dense.shape, dense.dtype),
        in_specs=[pl.BlockSpec(memory_space=pltpu.VMEM)],
        out_specs=pl.BlockSpec(memory_space=pltpu.VMEM),
        scratch_shapes=[
            pltpu.SemaphoreType.DMA((n,)),
            pltpu.SemaphoreType.DMA((n,)),
            pltpu.SemaphoreType.DMA,
        ],
        compiler_params=pltpu.CompilerParams(collective_id=number, has_side_effects=True),
        name=("dispatch", "combine")[number],
    )(dense).reshape(blocks.shape)


def shards(
    tokens,
    lengths,
    latent_cache,
    rotary_cache,
    route_ids,
    route_scores,
    attn_gain,
    w_query_down,
    query_gain,
    w_query_nope,
    w_query_rope,
    w_key_absorb,
    latent_gain,
    w_latent_down,
    w_rotary_key,
    w_value_up,
    w_output,
    ffn_gain,
    expert_gate,
    expert_up,
    expert_down,
    shared_gate,
    shared_up,
    shared_down,
):
    f32 = jnp.float32
    bf16 = jnp.bfloat16
    rows, model = tokens.shape
    heads, nope, latent = w_key_absorb.shape
    rotary = w_rotary_key.shape[1]
    top = route_ids.shape[1]
    normed = rms_scale(tokens.astype(f32), attn_gain).astype(bf16)
    query_low = rms_scale(
        jnp.dot(normed, w_query_down, preferred_element_type=f32), query_gain
    ).astype(bf16)
    query_nope = (
        jnp.dot(query_low, w_query_nope, preferred_element_type=f32)
        .astype(bf16)
        .reshape(rows, heads, nope)
    )
    query_rot = jnp.dot(query_low, w_query_rope, preferred_element_type=f32).reshape(
        rows, heads, rotary
    )
    query_rot = rotate(query_rot, lengths).astype(bf16)
    query_lat = jnp.einsum(
        "thn,hnl->thl", query_nope, w_key_absorb, preferred_element_type=f32
    ).astype(bf16)
    latent_new = rms_scale(
        jnp.dot(normed, w_latent_down, preferred_element_type=f32), latent_gain
    ).astype(bf16)
    rotary_new = rotate(jnp.dot(normed, w_rotary_key, preferred_element_type=f32), lengths).astype(
        bf16
    )
    scale = (nope + rotary) ** (-0.5)
    scores = (
        jnp.einsum("thl,tkl->thk", query_lat, latent_cache, preferred_element_type=f32)
        + jnp.einsum("thr,tkr->thk", query_rot, rotary_cache, preferred_element_type=f32)
    ) * scale
    live = jnp.arange(latent_cache.shape[1], dtype=jnp.int32)[None, :] < lengths[:, None]
    scores = jnp.where(live[:, None, :], scores, -jnp.inf)
    own = (
        jnp.einsum("thl,tl->th", query_lat, latent_new, preferred_element_type=f32)
        + jnp.einsum("thr,tr->th", query_rot, rotary_new, preferred_element_type=f32)
    ) * scale
    highest = jnp.maximum(jnp.max(scores, axis=-1), own)
    weights = jnp.exp(scores - highest[..., None])
    own_weight = jnp.exp(own - highest)
    total = jnp.sum(weights, axis=-1) + own_weight
    probs = (weights / total[..., None]).astype(bf16)
    own_prob = (own_weight / total).astype(bf16)
    out_lat = jnp.einsum("thk,tkl->thl", probs, latent_cache, preferred_element_type=f32)
    out_lat = (
        out_lat + own_prob.astype(f32)[..., None] * latent_new.astype(f32)[:, None, :]
    ).astype(bf16)
    values = jnp.einsum("thl,hlv->thv", out_lat, w_value_up, preferred_element_type=f32).astype(
        bf16
    )
    values = values.reshape(rows, model)
    attended = jnp.dot(
        values, lax.all_gather(w_output, "ep", axis=1, tiled=True), preferred_element_type=f32
    ).astype(bf16)
    residual = (tokens.astype(f32) + attended.astype(f32)).astype(bf16)
    ffn_in = rms_scale(residual.astype(f32), ffn_gain).astype(bf16)
    devices = lax.axis_size("ep")
    local_experts = expert_gate.shape[0]
    experts = devices * local_experts
    capacity = max(2, rows * top * 8 // (3 * experts))
    flat_ids = route_ids.reshape(-1)
    hits = (flat_ids[:, None] == jnp.arange(experts, dtype=jnp.int32)[None, :]).astype(jnp.int32)
    earlier = jnp.cumsum(hits, axis=0) - hits
    slot = jnp.sum(earlier * hits, axis=1)
    target = flat_ids * capacity + slot
    slot_range = jnp.arange(experts * capacity, dtype=jnp.int32)
    per_token = jnp.any(
        slot_range[:, None, None] == target.reshape(rows, top)[None, :, :], axis=2
    ).astype(bf16)
    per_pair = (target[:, None] == slot_range[None, :]).astype(bf16)
    outgoing = (
        jnp.dot(per_token, ffn_in, preferred_element_type=f32)
        .astype(bf16)
        .reshape(experts, capacity, model)
    )
    count = capacity
    arrived = exchange(outgoing.reshape(devices, local_experts * count, model), 0)
    grouped = arrived.reshape(devices, local_experts, count, model)
    gate = jnp.einsum("sjcd,jdf->sjcf", grouped, expert_gate, preferred_element_type=f32)
    upward = jnp.einsum("sjcd,jdf->sjcf", grouped, expert_up, preferred_element_type=f32)
    hidden = (jax.nn.silu(gate) * upward).astype(bf16)
    result = jnp.einsum("sjcf,jfd->sjcd", hidden, expert_down, preferred_element_type=f32).astype(
        bf16
    )
    returned = exchange(result.reshape(devices, local_experts * count, model), 1)
    picked = jnp.dot(
        per_pair, returned.reshape(experts * capacity, model), preferred_element_type=f32
    )
    route_weight = ROUTED_SCALE * route_scores / jnp.sum(route_scores, axis=1, keepdims=True)
    routed = jnp.sum(picked.reshape(rows, top, model) * route_weight[:, :, None], axis=1)
    gate_shared = jnp.dot(ffn_in, shared_gate, preferred_element_type=f32)
    up_shared = jnp.dot(ffn_in, shared_up, preferred_element_type=f32)
    hidden_shared = (jax.nn.silu(gate_shared) * up_shared).astype(bf16)
    shared_out = jnp.dot(hidden_shared, shared_down, preferred_element_type=f32)
    mixed = (residual.astype(f32) + routed + shared_out).astype(bf16)
    return (mixed, latent_new, rotary_new)


def solution(mesh):
    return jax.shard_map(
        shards,
        mesh=mesh,
        in_specs=(
            P("ep", None),
            P("ep"),
            P("ep", None, None),
            P("ep", None, None),
            P("ep", None),
            P("ep", None),
            P(),
            P(),
            P(),
            P(),
            P(),
            P(),
            P(),
            P(),
            P(),
            P(),
            P(None, "ep"),
            P(),
            P("ep", None, None),
            P("ep", None, None),
            P("ep", None, None),
            P(),
            P(),
            P(),
        ),
        out_specs=(P("ep", None), P("ep", None), P("ep", None)),
        check_vma=False,
    )
```
